32 devices in a mesh: sp: 8 (over z, x), tp: 4 (over y, core).
Axes of the slice: x: 2, y: 2, z: 4, core: 2. Of those that a mesh axis runs over, the one named last changes fastest.
Arguments:
- prompt: bfloat16 [4, 4096, 4096], P(None, 'sp'), may hold values from -6 to 6
- key_weight: bfloat16 [4096, 1024], P(None, 'tp'), may hold values from -0.09375 to 0.09375
- value_weight: bfloat16 [4096, 2048], P(None, 'tp'), may hold values from -0.09375 to 0.09375
- input_gate_weight: bfloat16 [4096, 16], P(None, 'tp'), may hold values from -0.09375 to 0.09375
- forget_gate_weight: bfloat16 [4096, 16], P(None, 'tp'), may hold values from -0.09375 to 0.09375
- forget_bias: float32 [16], P('tp'), may hold values from 3 to 11
- key_taps: bfloat16 [3, 1024], P(None, 'tp'), may hold values from -3 to 3
- extra_decay: float32 [4, 4096, 16], P(None, 'sp', 'tp'), may hold values from -1.5 to 0
- new_query: bfloat16 [4, 16, 64], P(None, 'tp'), may hold values from -6 to 6
- new_key: bfloat16 [4, 16, 64], P(None, 'tp'), may hold values from -6 to 6
- new_value: bfloat16 [4, 16, 128], P(None, 'tp', 'sp'), may hold values from -6 to 6
- new_input_gate: float32 [4, 16], P(None, 'tp'), may hold values from 2 to 7
- new_forget_gate: float32 [4, 16], P(None, 'tp'), may hold values from -2 to 4
- out_weight: bfloat16 [16, 128, 4096], P('tp', 'sp'), may hold values from -0.125 to 0.125
Outputs:
- cache_memory: bfloat16 [4, 16, 64, 128], P(None, 'tp', None, 'sp')
- cache_norm: bfloat16 [4, 16, 64], P(None, 'tp', 'sp')
- cache_peak: float32 [4, 16], P(None, 'tp')
- read_out: bfloat16 [4, 4096], P(None, ('sp', 'tp'))
The draws below stay inside these ranges and needn't reach their ends.
All inputs are finite; a program needn't handle non-finite values.
Results may differ from the reference program's by a relative error of at most 0.012.
The reference program's roundings to bfloat16 on the way count: a program that leaves them out, or rounds other values in their place, can miss the bound.
Values may be sent and summed in bfloat16 or wider, within the bound.
A program may use at most 64 MiB of HBM per device.

```python
import math
import jax
import jax.numpy as jnp
from jax import lax

D = 4096
HEAD_TOTAL = 16
KEY_DIM = 64
VALUE_DIM = 128
TAPS = 3
PROMPT_COUNT = 4
SEG = 512
PROMPT_LENGTH = 4096


def draw_forget_bias(key, part):
    first_key, second_key, third_key = jax.random.split(key, 3)
    chooser = jax.random.uniform(first_key, (HEAD_TOTAL,), jnp.float32)
    share = 0.5
    quick_bias = jax.random.uniform(second_key, (HEAD_TOTAL,), jnp.float32, 3.0, 4.2)
    steady_bias = jnp.log(jnp.float32(PROMPT_LENGTH)) + jax.random.uniform(third_key, (HEAD_TOTAL,), jnp.float32, 1.5, 3.0)
    steady_bias = jnp.minimum(steady_bias, 11.0)
    return jnp.where(chooser < share, quick_bias, steady_bias)


def draw_extra_decay(key, part):
    key_seg, key_location, key_depth = jax.random.split(key, 3)
    blocks = PROMPT_LENGTH // SEG
    seg_log = jax.random.uniform(key_seg, (PROMPT_COUNT, blocks, HEAD_TOTAL), jnp.float32, math.log(0.005), math.log(0.05))
    stable_offset = jnp.repeat(-jnp.exp(seg_log) / SEG, SEG, axis=1)
    spike_location = jax.random.randint(key_location, (PROMPT_COUNT, 2, HEAD_TOTAL), 0, PROMPT_LENGTH)
    depth_limit = jax.random.uniform(key_depth, (PROMPT_COUNT, 2, HEAD_TOTAL), jnp.float32, 0.22, 0.7)
    token_position = jnp.arange(PROMPT_LENGTH)
    hit_values = token_position[None, :, None, None] == spike_location[:, None, :, :]
    spike_values = jnp.sum(jnp.where(hit_values, -depth_limit[:, None, :, :], 0.0), axis=2)
    return stable_offset + spike_values


def levels(key, dims, pieces, smallest, top_value):
    gain = 1.0
    for dim, parts in pieces:
        draws = jax.random.uniform(jax.random.fold_in(jax.random.fold_in(key, 6), dim), (parts,), jnp.float32, smallest / len(pieces), top_value / len(pieces))
        gain = gain * jnp.repeat(jnp.exp(draws), dims[dim] // parts).reshape((-1,) + (1,) * (len(dims) - 1 - dim))
    return gain


def scatter_about(own_key, shape, width, limit, shards=(), held_as=jnp.bfloat16):
    level = levels(own_key, shape, shards, -0.22, 0.18) if shards else 1.0
    drawn = jax.random.normal(own_key, shape, jnp.float32) * width * level
    return jnp.minimum(jnp.maximum(drawn, -limit), limit).astype(held_as)


def setup_inputs(seed: int = 0) -> dict:
    seeds = jax.random.split(jax.random.key(seed), 15)
    prompt = scatter_about(seeds[0], (PROMPT_COUNT, PROMPT_LENGTH, D), 1.0, 6.0, ((1, 8),))
    key_weight = scatter_about(seeds[1], (D, HEAD_TOTAL * KEY_DIM), D ** -0.5, 0.09375, ((1, 4),))
    value_weight = scatter_about(seeds[2], (D, HEAD_TOTAL * VALUE_DIM), D ** -0.5, 0.09375, ((1, 4),))
    input_gate_weight = scatter_about(seeds[3], (D, HEAD_TOTAL), D ** -0.5, 0.09375, ((1, 4),))
    forget_gate_weight = scatter_about(seeds[4], (D, HEAD_TOTAL), D ** -0.5, 0.09375, ((1, 4),))
    forget_bias = draw_forget_bias(jax.random.fold_in(seeds[14], 71), 0)
    key_taps = scatter_about(seeds[6], (TAPS, HEAD_TOTAL * KEY_DIM), 0.577, 3.0, ((1, 4),))
    extra_decay = draw_extra_decay(jax.random.fold_in(seeds[14], 71), 0)
    new_query = scatter_about(seeds[8], (PROMPT_COUNT, HEAD_TOTAL, KEY_DIM), 1.0, 6.0, ((1, 4),))
    new_key = scatter_about(seeds[9], (PROMPT_COUNT, HEAD_TOTAL, KEY_DIM), 1.0, 6.0, ((1, 4),))
    new_value = scatter_about(seeds[10], (PROMPT_COUNT, HEAD_TOTAL, VALUE_DIM), 1.0, 6.0, ((1, 4), (2, 8)))
    new_input_gate = jnp.clip(2.0 + 5.0 * jax.random.uniform(seeds[11], (PROMPT_COUNT, HEAD_TOTAL), jnp.float32) ** levels(seeds[11], (PROMPT_COUNT, HEAD_TOTAL), ((1, 4),), -0.2, 0.2), 2.0, 7.0)
    new_forget_gate = jnp.clip(-2.0 + 6.0 * jax.random.uniform(seeds[12], (PROMPT_COUNT, HEAD_TOTAL), jnp.float32) ** levels(seeds[12], (PROMPT_COUNT, HEAD_TOTAL), ((1, 4),), -0.2, 0.2), -2.0, 4.0)
    out_weight = scatter_about(seeds[13], (HEAD_TOTAL, VALUE_DIM, D), (HEAD_TOTAL * VALUE_DIM) ** -0.5, 0.125, ((0, 4), (1, 8)))
    return dict(prompt=prompt, key_weight=key_weight, value_weight=value_weight, input_gate_weight=input_gate_weight, forget_gate_weight=forget_gate_weight, forget_bias=forget_bias, key_taps=key_taps, extra_decay=extra_decay, new_query=new_query, new_key=new_key, new_value=new_value, new_input_gate=new_input_gate, new_forget_gate=new_forget_gate, out_weight=out_weight)


def widen(rounded):
    return lax.optimization_barrier(rounded).astype(jnp.float32)


def key_conv(key_raw, key_taps):
    padded = jnp.pad(key_raw, ((1, 1), (0, 0)))
    tap_f32 = key_taps.astype(jnp.float32)
    mixed = tap_f32[0] * padded[:-2] + tap_f32[1] * padded[1:-1] + tap_f32[2] * padded[2:]
    return (jax.nn.silu(mixed) * KEY_DIM ** -0.5).astype(jnp.bfloat16)


def reference(prompt, key_weight, value_weight, input_gate_weight, forget_gate_weight, forget_bias,
              key_taps, extra_decay, new_query, new_key, new_value, new_input_gate, new_forget_gate,
              out_weight):
    def prompt_state(inputs):
        seq_rows, seq_extra = inputs
        key_raw = jnp.dot(seq_rows, key_weight, preferred_element_type=jnp.float32).astype(jnp.bfloat16)
        values = jnp.dot(seq_rows, value_weight, preferred_element_type=jnp.float32).astype(jnp.bfloat16)
        input_pre = widen(jnp.dot(seq_rows, input_gate_weight, preferred_element_type=jnp.float32).astype(jnp.bfloat16))
        forget_pre = widen(jnp.dot(seq_rows, forget_gate_weight, preferred_element_type=jnp.float32).astype(jnp.bfloat16))
        key_rows = key_conv(key_raw, key_taps)
        log_forget = jax.nn.log_sigmoid(forget_pre + forget_bias) + seq_extra
        suffix = jnp.sum(log_forget, axis=0, keepdims=True) - jnp.cumsum(log_forget, axis=0)
        gate_log = input_pre + suffix
        peak_log = jnp.max(gate_log, axis=0)
        scale = jnp.exp(gate_log - peak_log[None])
        key_quartet = key_rows.reshape(PROMPT_LENGTH, HEAD_TOTAL, KEY_DIM).astype(jnp.float32)
        value_four = values.reshape(PROMPT_LENGTH, HEAD_TOTAL, VALUE_DIM)
        weighted_rows = (value_four * scale[:, :, None]).astype(jnp.bfloat16)
        memory_matrix = jnp.einsum('xje,xjb->jeb', key_quartet, weighted_rows.astype(jnp.float32))
        normer = jnp.einsum('lh,lhk->hk', scale, key_quartet, precision=lax.Precision.HIGHEST)
        return memory_matrix, normer, peak_log

    memory_matrix, normer, peak_log = lax.map(prompt_state, (prompt, extra_decay))
    forget_new = jax.nn.log_sigmoid(new_forget_gate)
    new_peak = jnp.maximum(forget_new + peak_log, new_input_gate)
    old_scale = jnp.exp(forget_new + peak_log - new_peak)
    new_scale = jnp.exp(new_input_gate - new_peak)
    key_new = new_key.astype(jnp.float32)
    value_new = new_value.astype(jnp.float32)
    memory_next = (old_scale[:, :, None, None] * memory_matrix
                   + new_scale[:, :, None, None] * key_new[:, :, :, None] * value_new[:, :, None, :])
    normer_next = old_scale[:, :, None] * normer + new_scale[:, :, None] * key_new
    query = new_query.astype(jnp.float32)
    numer = jnp.sum(query[:, :, :, None] * memory_next, axis=2)
    denom = jnp.sum(query * normer_next, axis=-1)
    read = (numer / jnp.maximum(jnp.abs(denom), 1.0)[:, :, None]).astype(jnp.bfloat16)
    read_out = jnp.dot(read.reshape(PROMPT_COUNT, HEAD_TOTAL * VALUE_DIM), out_weight.reshape(HEAD_TOTAL * VALUE_DIM, D),
                       preferred_element_type=jnp.float32).astype(jnp.bfloat16)
    return memory_matrix.astype(jnp.bfloat16), normer.astype(jnp.bfloat16), peak_log, read_out
```

```python
import functools

import jax
import jax.numpy as jnp
from jax import lax
from jax.experimental import pallas as pl
from jax.experimental.pallas import tpu as pltpu
from jax.sharding import PartitionSpec as P

EDGE = 16
EXTRA_ROWS = 8


def log_sigmoid(x):
    return jnp.minimum(x, 0.0) - jnp.log1p(jnp.exp(-jnp.abs(x)))


def three_parts(x):
    high = x.astype(jnp.bfloat16)
    rest = x - high.astype(jnp.float32)
    middle = rest.astype(jnp.bfloat16)
    low = (rest - middle.astype(jnp.float32)).astype(jnp.bfloat16)
    return jnp.concatenate([high, middle, low], axis=1)


def kernel(
    sp_count,
    tp_count,
    prompt,
    key_weight,
    value_weight,
    out_weight,
    gate_weight,
    bias,
    taps,
    extra,
    small,
    new_value,
    memory_out,
    norm_out,
    peak_out,
    read_out,
    rows,
    edges,
    wk,
    wv,
    wo,
    later,
    padded,
    values,
    gates,
    share,
    shares,
    halo_out,
    halo_in,
    parts_out,
    parts_in,
    row_sem,
    edge_sem,
    weight_sem,
    share_send,
    share_recv,
    halo_send,
    halo_recv,
    part_send,
    part_recv,
):
    seqs, seg, width = rows.shape
    lanes = wk.shape[1]
    heads = bias.shape[1]
    key_size = lanes // heads
    value_size = wv.shape[1] // heads
    cols = value_size // sp_count
    total = sp_count * tp_count
    sp, tp = lax.axis_index("sp"), lax.axis_index("tp")
    me = sp * tp_count + tp
    f32, bf16 = jnp.float32, jnp.bfloat16

    def device(j):
        return {"sp": j // tp_count, "tp": lax.rem(j, tp_count)}

    barrier = pltpu.get_barrier_semaphore()

    def greet(o, carry):
        j = lax.rem(me + o, total)
        pl.semaphore_signal(
            barrier, inc=1, device_id=device(j), device_id_type=pl.DeviceIdType.MESH
        )
        return carry

    key_copy = pltpu.make_async_copy(key_weight, wk, weight_sem.at[0])
    value_copy = pltpu.make_async_copy(value_weight, wv, weight_sem.at[1])
    out_copy = pltpu.make_async_copy(out_weight, wo, weight_sem.at[2])
    edge_copies = [
        pltpu.make_async_copy(
            prompt.at[s, pl.ds(start, EDGE)], edges.at[2 * s + side], edge_sem.at[2 * s + side]
        )
        for s in range(seqs)
        for side, start in enumerate((0, seg - EDGE))
    ]
    key_copy.start()
    for copy in edge_copies:
        copy.start()
    pltpu.make_async_copy(prompt.at[0], rows.at[0], row_sem.at[0]).start()
    value_copy.start()
    for s in range(1, seqs):
        pltpu.make_async_copy(prompt.at[s], rows.at[s], row_sem.at[s]).start()
    out_copy.start()
    lax.fori_loop(1, total, greet, 0)

    place = lax.broadcasted_iota(jnp.int32, (seg, seg), 0)
    other = lax.broadcasted_iota(jnp.int32, (seg, seg), 1)
    later[...] = jnp.where(other > place, 1.0, 0.0).astype(bf16)

    for copy in edge_copies:
        copy.wait()
    key_copy.wait()
    edge_keys = jnp.dot(
        edges[...].reshape(2 * seqs * EDGE, width), wk[...], preferred_element_type=f32
    )
    edge_keys = edge_keys.astype(bf16).astype(f32)
    for s in range(seqs):
        first = 2 * s * EDGE
        last = first + 2 * EDGE - 1
        halo_out[0, s : s + 1, :] = edge_keys[last : last + 1]
        halo_out[1, s : s + 1, :] = edge_keys[first : first + 1]
    pl.semaphore_wait(barrier, total - 1)
    after = lax.rem(sp + 1, sp_count)
    before = lax.rem(sp + sp_count - 1, sp_count)
    halo_copies = [
        pltpu.make_async_remote_copy(
            src_ref=halo_out.at[i],
            dst_ref=halo_in.at[i],
            send_sem=halo_send.at[i],
            recv_sem=halo_recv.at[i],
            device_id={"sp": to, "tp": tp},
            device_id_type=pl.DeviceIdType.MESH,
        )
        for i, to in enumerate((after, before))
    ]
    for copy in halo_copies:
        copy.start()
    value_copy.wait()

    lane_head = lax.broadcasted_iota(jnp.int32, (1, lanes), 1) // key_size
    tap = taps[...].astype(f32)

    def by_head(x):
        out = jnp.zeros((x.shape[0], lanes), f32)
        for h in range(heads):
            out = jnp.where(lane_head == h, x[:, h : h + 1], out)
        return out

    def share_copy(s, q):
        return pltpu.make_async_remote_copy(
            src_ref=share.at[s, q],
            dst_ref=shares.at[s, sp],
            send_sem=share_send.at[s, q],
            recv_sem=share_recv.at[s, sp],
            device_id={"sp": q, "tp": tp},
            device_id_type=pl.DeviceIdType.MESH,
        )

    block = min(256, seg)

    def project(i, s):
        at = pl.ds(pl.multiple_of(i * block, block), block)
        x = rows[s, at, :]
        key_raw = jnp.dot(x, wk[...], preferred_element_type=f32)
        padded[pl.ds(pl.multiple_of(i * block + 8, 8), block), :] = key_raw.astype(bf16).astype(f32)
        values[at, :] = jnp.dot(x, wv[...], preferred_element_type=f32).astype(bf16)
        gate = jnp.dot(x, gate_weight[...], preferred_element_type=f32)
        gates[at, :] = gate.astype(bf16).astype(f32)
        return s

    def sequence(s, carry):
        pltpu.make_async_copy(prompt.at[s], rows.at[s], row_sem.at[s]).wait()
        lax.fori_loop(0, seg // block, project, s)

        @pl.when(s == 0)
        def _():
            for copy in halo_copies:
                copy.wait()

        zero = jnp.zeros((1, lanes), f32)
        padded[7:8, :] = jnp.where(sp == 0, zero, halo_in[0, pl.ds(s, 1), :])
        padded[seg + 8 : seg + 9, :] = jnp.where(
            sp == sp_count - 1, zero, halo_in[1, pl.ds(s, 1), :]
        )
        mixed = (
            tap[0:1] * padded[7 : seg + 7, :]
            + tap[1:2] * padded[8 : seg + 8, :]
            + tap[2:3] * padded[9 : seg + 9, :]
        )
        key_rows = (mixed * jax.nn.sigmoid(mixed) * key_size ** (-0.5)).astype(bf16)

        gate = gates[...]
        log_forget = log_sigmoid(gate[:, :heads] + bias[...]) + extra[s]
        sums = jnp.dot(later[...], three_parts(log_forget), preferred_element_type=f32)
        suffix = sums[:, :heads] + sums[:, heads : 2 * heads] + sums[:, 2 * heads :]
        gate_log = gate[:, heads:] + suffix
        seg_total = jnp.sum(log_forget, axis=0, keepdims=True)
        top = jnp.max(gate_log, axis=0, keepdims=True)
        scale = jnp.exp(gate_log - top)

        over = (((0,), (0,)), ((), ()))
        memory = jnp.zeros((value_size, lanes), f32)
        for h in range(heads):
            value = values[:, h * value_size : (h + 1) * value_size].astype(f32)
            weighted = (value * scale[:, h : h + 1]).astype(bf16)
            outer = lax.dot_general(weighted, key_rows, over, preferred_element_type=f32)
            memory = jnp.where(lane_head == h, outer, memory)
        normers = lax.dot_general(
            three_parts(scale), key_rows, over, preferred_element_type=f32
        )
        row_head = lax.rem(lax.broadcasted_iota(jnp.int32, normers.shape, 0), heads)
        normer = jnp.sum(jnp.where(row_head == lane_head, normers, 0.0), axis=0, keepdims=True)
        row = lax.broadcasted_iota(jnp.int32, (EXTRA_ROWS, lanes), 0)
        extras = jnp.where(row == 0, normer, jnp.where(row == 1, by_head(seg_total), by_head(top)))
        for q in range(sp_count):
            share[s, q, :cols, :] = memory[q * cols : (q + 1) * cols]
            share[s, q, cols:, :] = extras
        shares[s, sp] = share[s, sp]

        def send(o, c):
            share_copy(s, lax.rem(sp + o, sp_count)).start()
            return c

        return lax.fori_loop(1, sp_count, send, carry)

    lax.fori_loop(0, seqs, sequence, 0)
    out_copy.wait()

    def arrive(i, c):
        s = i // (sp_count - 1)
        q = lax.rem(sp + 1 + lax.rem(i, sp_count - 1), sp_count)
        pltpu.make_async_remote_copy(
            src_ref=share.at[s, q],
            dst_ref=shares.at[s, q],
            send_sem=share_send.at[s, q],
            recv_sem=share_recv.at[s, q],
            device_id={"sp": q, "tp": tp},
            device_id_type=pl.DeviceIdType.MESH,
        ).wait()
        return c

    lax.fori_loop(0, seqs * (sp_count - 1), arrive, 0)

    depth = heads * cols
    lane = lax.broadcasted_iota(jnp.int32, (depth, 128), 1)
    reads = jnp.zeros((depth, 128), f32)
    for s in range(seqs):
        pieces = [shares[s, d] for d in range(sp_count)]
        tail = jnp.zeros((1, lanes), f32)
        tops = [None] * sp_count
        for d in reversed(range(sp_count)):
            tops[d] = pieces[d][cols + 2 : cols + 3] + tail
            tail = tail + pieces[d][cols + 1 : cols + 2]
        peak = functools.reduce(jnp.maximum, tops)
        memory = jnp.zeros((cols, lanes), f32)
        normer = jnp.zeros((1, lanes), f32)
        for d in range(sp_count):
            factor = jnp.exp(tops[d] - peak)
            memory = memory + factor * pieces[d][:cols]
            normer = normer + factor * pieces[d][cols : cols + 1]
        memory_out[s] = memory
        norm_out[s : s + 1, :] = normer
        peak_out[s : s + 1, :] = peak
        query, key = small[0, s : s + 1, :], small[1, s : s + 1, :]
        input_new, forget_new = small[2, s : s + 1, :], log_sigmoid(small[3, s : s + 1, :])
        new_peak = jnp.maximum(forget_new + peak, input_new)
        old_scale = jnp.exp(forget_new + peak - new_peak)
        new_scale = jnp.exp(input_new - new_peak)
        numer = query * (old_scale * memory + new_scale * key * new_value[s])
        denom = query * (old_scale * normer + new_scale * key)
        found = []
        for h in range(heads):
            top = jnp.sum(jnp.where(lane_head == h, numer, 0.0), axis=1, keepdims=True)
            under = jnp.sum(jnp.where(lane_head == h, denom, 0.0), axis=1, keepdims=True)
            found.append(top / jnp.maximum(jnp.abs(under), 1.0))
        reads = jnp.where(lane == s, jnp.concatenate(found, axis=0), reads)
    if depth < 128:
        reads = jnp.concatenate([reads, jnp.zeros((128 - depth, 128), f32)], axis=0)
    left = reads.T[:8, :depth].astype(bf16)
    partial = jnp.dot(left, wo[...], preferred_element_type=f32)
    features = read_out.shape[1]
    for j in range(total):
        parts_out[j] = partial[:seqs, j * features : (j + 1) * features]
    parts_in[me] = parts_out[me]

    def part_copy(j, slot):
        return pltpu.make_async_remote_copy(
            src_ref=parts_out.at[j],
            dst_ref=parts_in.at[slot],
            send_sem=part_send.at[j],
            recv_sem=part_recv.at[slot],
            device_id=device(j),
            device_id_type=pl.DeviceIdType.MESH,
        )

    def send_part(o, c):
        part_copy(lax.rem(me + o, total), me).start()
        return c

    def take_part(o, c):
        j = lax.rem(me + o, total)
        part_copy(j, j).wait()
        return c

    lax.fori_loop(1, total, send_part, 0)
    lax.fori_loop(1, total, take_part, 0)
    read_out[...] = jnp.sum(parts_in[...], axis=0).astype(bf16)


def body(
    prompt,
    key_weight,
    value_weight,
    input_gate_weight,
    forget_gate_weight,
    forget_bias,
    key_taps,
    extra_decay,
    new_query,
    new_key,
    new_value,
    new_input_gate,
    new_forget_gate,
    out_weight,
):
    f32, bf16 = jnp.float32, jnp.bfloat16
    sp_count, tp_count = lax.axis_size("sp"), lax.axis_size("tp")
    total = sp_count * tp_count
    seqs, seg, width = prompt.shape
    heads, key_size = new_key.shape[1:]
    lanes = heads * key_size
    cols = new_value.shape[2]
    value_width = value_weight.shape[1]
    depth = heads * cols
    out_width = out_weight.shape[2]
    features = out_width // total

    def by_lane(x):
        return jnp.repeat(x.astype(f32), key_size, axis=-1)

    small = jnp.stack(
        [
            new_query.reshape(seqs, lanes).astype(f32),
            new_key.reshape(seqs, lanes).astype(f32),
            by_lane(new_input_gate),
            by_lane(new_forget_gate),
        ]
    )
    value_lanes = by_lane(new_value.transpose(0, 2, 1))
    gate_weight = jnp.concatenate([forget_gate_weight, input_gate_weight], axis=1)
    vmem = pl.BlockSpec(memory_space=pltpu.VMEM)
    hbm = pl.BlockSpec(memory_space=pl.ANY)
    block_rows = cols + EXTRA_ROWS
    memory, normer, peak, read = pl.pallas_call(
        functools.partial(kernel, sp_count, tp_count),
        out_shape=(
            jax.ShapeDtypeStruct((seqs, cols, lanes), f32),
            jax.ShapeDtypeStruct((seqs, lanes), f32),
            jax.ShapeDtypeStruct((seqs, lanes), f32),
            jax.ShapeDtypeStruct((seqs, features), bf16),
        ),
        in_specs=[hbm] * 4 + [vmem] * 6,
        out_specs=[vmem] * 4,
        scratch_shapes=[
            pltpu.VMEM((seqs, seg, width), bf16),
            pltpu.VMEM((2 * seqs, EDGE, width), bf16),
            pltpu.VMEM((width, lanes), bf16),
            pltpu.VMEM((width, value_width), bf16),
            pltpu.VMEM((depth, out_width), bf16),
            pltpu.VMEM((seg, seg), bf16),
            pltpu.VMEM((seg + 16, lanes), f32),
            pltpu.VMEM((seg, value_width), bf16),
            pltpu.VMEM((seg, 2 * heads), f32),
            pltpu.VMEM((seqs, sp_count, block_rows, lanes), f32),
            pltpu.VMEM((seqs, sp_count, block_rows, lanes), f32),
            pltpu.VMEM((2, seqs, lanes), f32),
            pltpu.VMEM((2, seqs, lanes), f32),
            pltpu.VMEM((total, seqs, features), f32),
            pltpu.VMEM((total, seqs, features), f32),
            pltpu.SemaphoreType.DMA((seqs,)),
            pltpu.SemaphoreType.DMA((2 * seqs,)),
            pltpu.SemaphoreType.DMA((3,)),
            pltpu.SemaphoreType.DMA((seqs, sp_count)),
            pltpu.SemaphoreType.DMA((seqs, sp_count)),
            pltpu.SemaphoreType.DMA((2,)),
            pltpu.SemaphoreType.DMA((2,)),
            pltpu.SemaphoreType.DMA((total,)),
            pltpu.SemaphoreType.DMA((total,)),
        ],
        compiler_params=pltpu.CompilerParams(
            collective_id=0, has_side_effects=True, vmem_limit_bytes=60 * 2**20
        ),
    )(
        prompt,
        key_weight,
        value_weight,
        out_weight.reshape(depth, out_width),
        gate_weight,
        forget_bias.reshape(1, heads),
        key_taps,
        extra_decay,
        small,
        value_lanes,
    )
    memory = memory.reshape(seqs, cols, heads, key_size).transpose(0, 2, 3, 1)
    key_cols = key_size // sp_count
    normer = lax.dynamic_slice_in_dim(
        normer.reshape(seqs, heads, key_size), lax.axis_index("sp") * key_cols, key_cols, 2
    )
    return (
        memory.astype(bf16),
        normer.astype(bf16),
        peak.reshape(seqs, heads, key_size)[:, :, 0],
        read,
    )


def solution(mesh):
    placed = (
        P(None, "sp", None),
        P(None, "tp"),
        P(None, "tp"),
        P(None, "tp"),
        P(None, "tp"),
        P("tp"),
        P(None, "tp"),
        P(None, "sp", "tp"),
        P(None, "tp", None),
        P(None, "tp", None),
        P(None, "tp", "sp"),
        P(None, "tp"),
        P(None, "tp"),
        P("tp", "sp", None),
    )
    return jax.shard_map(
        body,
        mesh=mesh,
        in_specs=placed,
        out_specs=(
            P(None, "tp", None, "sp"),
            P(None, "tp", "sp"),
            P(None, "tp"),
            P(None, ("sp", "tp")),
        ),
        check_vma=False,
    )
```

```python
import functools

import jax
import jax.numpy as jnp
from jax import lax
from jax.experimental import pallas as pl
from jax.experimental.pallas import tpu as pltpu
from jax.sharding import PartitionSpec as P

EDGE = 16
NOTE_ROWS = 4


def log_sigmoid(x):
    return jnp.minimum(x, 0.0) - jnp.log1p(jnp.exp(-jnp.abs(x)))


def three_parts(x):
    high = x.astype(jnp.bfloat16).astype(jnp.float32)
    rest = x - high
    middle = rest.astype(jnp.bfloat16).astype(jnp.float32)
    return jnp.concatenate([high, middle, rest - middle], axis=0).astype(jnp.bfloat16)


def kernel(
    sp_count,
    tp_count,
    prompt,
    key_weight,
    value_weight,
    out_weight,
    input_weight,
    forget_weight,
    bias,
    taps,
    extra,
    new_query,
    new_key,
    new_value,
    new_input,
    new_forget,
    memory_out,
    norm_out,
    peak_out,
    read_out,
    rows,
    edges,
    wk,
    wv,
    wo,
    wg,
    later,
    padded,
    values,
    gates,
    share,
    shares,
    note,
    notes,
    halo_out,
    halo_in,
    parts_out,
    parts_in,
    row_sem,
    edge_sem,
    weight_sem,
    share_send,
    share_recv,
    note_send,
    note_recv,
    halo_send,
    halo_recv,
    part_send,
    part_recv,
):
    seqs, seg, width = rows.shape
    lanes = wk.shape[1]
    heads = bias.shape[1]
    key_size = lanes // heads
    value_size = wv.shape[1] // heads
    cols = value_size // sp_count
    total = sp_count * tp_count
    sp, tp = lax.axis_index("sp"), lax.axis_index("tp")
    me = sp * tp_count + tp
    f32, bf16 = jnp.float32, jnp.bfloat16

    def device(j):
        return {"sp": j // tp_count, "tp": lax.rem(j, tp_count)}

    barrier = pltpu.get_barrier_semaphore()

    def greet(o, carry):
        j = lax.rem(me + o, total)
        pl.semaphore_signal(
            barrier, inc=1, device_id=device(j), device_id_type=pl.DeviceIdType.MESH
        )
        return carry

    key_copy = pltpu.make_async_copy(key_weight, wk, weight_sem.at[0])
    value_copy = pltpu.make_async_copy(value_weight, wv, weight_sem.at[1])
    out_copy = pltpu.make_async_copy(out_weight, wo, weight_sem.at[2])
    edge_copies = [
        pltpu.make_async_copy(
            prompt.at[s, pl.ds(start, EDGE)], edges.at[2 * s + side], edge_sem.at[2 * s + side]
        )
        for s in range(seqs)
        for side, start in enumerate((0, seg - EDGE))
    ]
    key_copy.start()
    for copy in edge_copies:
        copy.start()
    pltpu.make_async_copy(prompt.at[0], rows.at[0], row_sem.at[0]).start()
    value_copy.start()
    for s in range(1, seqs):
        pltpu.make_async_copy(prompt.at[s], rows.at[s], row_sem.at[s]).start()
    out_copy.start()
    lax.fori_loop(1, total, greet, 0)

    place = lax.broadcasted_iota(jnp.int32, (seg, seg), 0)
    other = lax.broadcasted_iota(jnp.int32, (seg, seg), 1)
    later[...] = jnp.where(place > other, 1.0, 0.0).astype(bf16)
    gate_rows = jnp.concatenate(
        [forget_weight[...].astype(f32), input_weight[...].astype(f32)], axis=0
    )
    wg[...] = gate_rows.T.astype(bf16)

    def column(x):
        size = x.shape[1]
        down = lax.broadcasted_iota(jnp.int32, (size, size), 0)
        across = lax.broadcasted_iota(jnp.int32, (size, size), 1)
        return jnp.sum(jnp.where(down == across, x, 0.0), axis=1, keepdims=True)

    bias_column = column(bias[...])

    for copy in edge_copies:
        copy.wait()
    key_copy.wait()
    edge_keys = jnp.dot(
        edges[...].reshape(2 * seqs * EDGE, width), wk[...], preferred_element_type=f32
    )
    edge_keys = edge_keys.astype(bf16).astype(f32)
    for s in range(seqs):
        first = 2 * s * EDGE
        last = first + 2 * EDGE - 1
        halo_out[0, s : s + 1, :] = edge_keys[last : last + 1]
        halo_out[1, s : s + 1, :] = edge_keys[first : first + 1]
    pl.semaphore_wait(barrier, total - 1)
    after = lax.rem(sp + 1, sp_count)
    before = lax.rem(sp + sp_count - 1, sp_count)
    halo_copies = [
        pltpu.make_async_remote_copy(
            src_ref=halo_out.at[i],
            dst_ref=halo_in.at[i],
            send_sem=halo_send.at[i],
            recv_sem=halo_recv.at[i],
            device_id={"sp": to, "tp": tp},
            device_id_type=pl.DeviceIdType.MESH,
        )
        for i, to in enumerate((after, before))
    ]
    for copy in halo_copies:
        copy.start()
    value_copy.wait()

    lane_head = lax.broadcasted_iota(jnp.int32, (1, lanes), 1) // key_size
    tap = taps[...].astype(f32)

    def by_head(x):
        out = jnp.zeros((x.shape[0], lanes), f32)
        for h in range(heads):
            out = jnp.where(lane_head == h, x[:, h : h + 1], out)
        return out

    def columns_by_head(x):
        row = lax.broadcasted_iota(jnp.int32, (heads, lanes), 0)
        return jnp.sum(jnp.where(row == lane_head, x, 0.0), axis=0, keepdims=True)

    def share_copy(s, q, slot):
        return pltpu.make_async_remote_copy(
            src_ref=share.at[s, q],
            dst_ref=shares.at[s, slot],
            send_sem=share_send.at[s, q],
            recv_sem=share_recv.at[s, slot],
            device_id={"sp": q, "tp": tp},
            device_id_type=pl.DeviceIdType.MESH,
        )

    def note_copy(s, q, slot):
        return pltpu.make_async_remote_copy(
            src_ref=note.at[s],
            dst_ref=notes.at[s, slot],
            send_sem=note_send.at[s, q],
            recv_sem=note_recv.at[s, slot],
            device_id={"sp": q, "tp": tp},
            device_id_type=pl.DeviceIdType.MESH,
        )

    block = min(256, seg)

    def project(i, s):
        at = pl.ds(pl.multiple_of(i * block, block), block)
        x = rows[s, at, :]
        key_raw = jnp.dot(x, wk[...], preferred_element_type=f32)
        padded[pl.ds(pl.multiple_of(i * block + 8, 8), block), :] = key_raw.astype(bf16).astype(f32)
        values[at, :] = jnp.dot(x, wv[...], preferred_element_type=f32).astype(bf16)
        gate = jnp.dot(x, wg[...], preferred_element_type=f32)
        gates[:, at] = gate.T.astype(bf16).astype(f32)
        return s

    def sequence(s, carry):
        pltpu.make_async_copy(prompt.at[s], rows.at[s], row_sem.at[s]).wait()
        lax.fori_loop(0, seg // block, project, s)

        @pl.when(s == 0)
        def _():
            for copy in halo_copies:
                copy.wait()

        zero = jnp.zeros((1, lanes), f32)
        padded[7:8, :] = jnp.where(sp == 0, zero, halo_in[0, pl.ds(s, 1), :])
        padded[seg + 8 : seg + 9, :] = jnp.where(
            sp == sp_count - 1, zero, halo_in[1, pl.ds(s, 1), :]
        )
        mixed = (
            tap[0:1] * padded[7 : seg + 7, :]
            + tap[1:2] * padded[8 : seg + 8, :]
            + tap[2:3] * padded[9 : seg + 9, :]
        )
        key_rows = (mixed * jax.nn.sigmoid(mixed) * key_size ** (-0.5)).astype(bf16)

        gate = gates[...]
        log_forget = log_sigmoid(gate[:heads] + bias_column) + extra[s]
        sums = jnp.dot(three_parts(log_forget), later[...], preferred_element_type=f32)
        suffix = sums[:heads] + sums[heads : 2 * heads] + sums[2 * heads :]
        gate_log = gate[heads:] + suffix
        seg_total = jnp.sum(log_forget, axis=1, keepdims=True)
        top = jnp.max(gate_log, axis=1, keepdims=True)
        scale = jnp.exp(gate_log - top)
        scale_columns = jnp.concatenate([scale, jnp.zeros((8 - heads, seg), f32)], axis=0).T

        over = (((0,), (0,)), ((), ()))
        memory = jnp.zeros((value_size, lanes), f32)
        for h in range(heads):
            value = values[:, h * value_size : (h + 1) * value_size].astype(f32)
            weighted = (value * scale_columns[:, h : h + 1]).astype(bf16)
            outer = lax.dot_general(weighted, key_rows, over, preferred_element_type=f32)
            memory = jnp.where(lane_head == h, outer, memory)
        normers = jnp.dot(three_parts(scale), key_rows, preferred_element_type=f32)
        row_head = lax.rem(lax.broadcasted_iota(jnp.int32, normers.shape, 0), heads)
        normer = jnp.sum(jnp.where(row_head == lane_head, normers, 0.0), axis=0, keepdims=True)
        note[s, 0:1, :] = normer
        note[s, 1:2, :] = columns_by_head(seg_total)
        note[s, 2:3, :] = columns_by_head(top)
        note[s, 3:4, :] = jnp.zeros((1, lanes), f32)
        for q in range(sp_count):
            share[s, q] = memory[q * cols : (q + 1) * cols].astype(bf16)
        shares[s, sp] = share[s, sp]
        notes[s, sp] = note[s]

        def send(o, c):
            q = lax.rem(sp + o, sp_count)
            note_copy(s, q, sp).start()
            share_copy(s, q, sp).start()
            return c

        return lax.fori_loop(1, sp_count, send, carry)

    lax.fori_loop(0, seqs, sequence, 0)
    out_copy.wait()

    def arrive(i, c):
        s = i // (sp_count - 1)
        q = lax.rem(sp + 1 + lax.rem(i, sp_count - 1), sp_count)
        note_copy(s, q, q).wait()
        share_copy(s, q, q).wait()
        return c

    queries, keys = (
        jnp.concatenate([ref[:, h, :].astype(f32) for h in range(heads)], axis=1)
        for ref in (new_query, new_key)
    )
    inputs = [by_head(new_input[s : s + 1, :]) for s in range(seqs)]
    forgets = [log_sigmoid(by_head(new_forget[s : s + 1, :])) for s in range(seqs)]
    fresh = []
    for s in range(seqs):
        out = jnp.zeros((cols, lanes), f32)
        for h in range(heads):
            out = jnp.where(lane_head == h, column(new_value[s, h : h + 1, :].astype(f32)), out)
        fresh.append(out)

    lax.fori_loop(0, seqs * (sp_count - 1), arrive, 0)

    depth = heads * cols
    lane = lax.broadcasted_iota(jnp.int32, (depth, 128), 1)
    reads = jnp.zeros((depth, 128), f32)
    for s in range(seqs):
        tail = jnp.zeros((1, lanes), f32)
        tops = [None] * sp_count
        for d in reversed(range(sp_count)):
            tops[d] = notes[s, d, 2:3, :] + tail
            tail = tail + notes[s, d, 1:2, :]
        peak = functools.reduce(jnp.maximum, tops)
        memory = jnp.zeros((cols, lanes), f32)
        normer = jnp.zeros((1, lanes), f32)
        for d in range(sp_count):
            factor = jnp.exp(tops[d] - peak)
            memory = memory + factor * shares[s, d].astype(f32)
            normer = normer + factor * notes[s, d, 0:1, :]
        key_cols = norm_out.shape[2]
        turned = pltpu.roll(
            jnp.broadcast_to(normer, (8, lanes)), lax.rem(lanes - sp * key_cols, lanes), 1
        )
        for h in range(heads):
            start = h * key_size
            memory_out[s, h] = memory[:, start : start + key_size]
            norm_out[s, h : h + 1, :] = turned[0:1, start : start + key_cols]
            peak_out[s : s + 1, h : h + 1] = peak[:, start : start + 1]
        query, key = queries[s : s + 1], keys[s : s + 1]
        input_new, forget_new = inputs[s], forgets[s]
        new_peak = jnp.maximum(forget_new + peak, input_new)
        old_scale = jnp.exp(forget_new + peak - new_peak)
        new_scale = jnp.exp(input_new - new_peak)
        numer = query * (old_scale * memory + new_scale * key * fresh[s])
        denom = query * (old_scale * normer + new_scale * key)
        found = []
        for h in range(heads):
            top = jnp.sum(jnp.where(lane_head == h, numer, 0.0), axis=1, keepdims=True)
            under = jnp.sum(jnp.where(lane_head == h, denom, 0.0), axis=1, keepdims=True)
            found.append(top / jnp.maximum(jnp.abs(under), 1.0))
        reads = jnp.where(lane == s, jnp.concatenate(found, axis=0), reads)
    if depth < 128:
        reads = jnp.concatenate([reads, jnp.zeros((128 - depth, 128), f32)], axis=0)
    left = reads.T[:8, :depth].astype(bf16)
    partial = jnp.dot(left, wo[...], preferred_element_type=f32)
    features = read_out.shape[1]
    for j in range(total):
        parts_out[j] = partial[:seqs, j * features : (j + 1) * features]
    parts_in[me] = parts_out[me]

    def part_copy(j, slot):
        return pltpu.make_async_remote_copy(
            src_ref=parts_out.at[j],
            dst_ref=parts_in.at[slot],
            send_sem=part_send.at[j],
            recv_sem=part_recv.at[slot],
            device_id=device(j),
            device_id_type=pl.DeviceIdType.MESH,
        )

    def send_part(o, c):
        part_copy(lax.rem(me + o, total), me).start()
        return c

    def take_part(o, c):
        j = lax.rem(me + o, total)
        part_copy(j, j).wait()
        return c

    lax.fori_loop(1, total, send_part, 0)
    lax.fori_loop(1, total, take_part, 0)
    read_out[...] = jnp.sum(parts_in[...], axis=0).astype(bf16)


def body(
    prompt,
    key_weight,
    value_weight,
    input_gate_weight,
    forget_gate_weight,
    forget_bias,
    key_taps,
    extra_decay,
    new_query,
    new_key,
    new_value,
    new_input_gate,
    new_forget_gate,
    out_weight,
):
    f32, bf16 = jnp.float32, jnp.bfloat16
    sp_count, tp_count = lax.axis_size("sp"), lax.axis_size("tp")
    total = sp_count * tp_count
    seqs, seg, width = prompt.shape
    heads, key_size = new_key.shape[1:]
    lanes = heads * key_size
    cols = new_value.shape[2]
    value_width = value_weight.shape[1]
    depth = heads * cols
    out_width = out_weight.shape[2]
    features = out_width // total

    vmem = pl.BlockSpec(memory_space=pltpu.VMEM)
    hbm = pl.BlockSpec(memory_space=pl.ANY)
    memory, normer, peak, read = pl.pallas_call(
        functools.partial(kernel, sp_count, tp_count),
        out_shape=(
            jax.ShapeDtypeStruct((seqs, heads, cols, key_size), f32),
            jax.ShapeDtypeStruct((seqs, heads, key_size // sp_count), f32),
            jax.ShapeDtypeStruct((seqs, heads), f32),
            jax.ShapeDtypeStruct((seqs, features), bf16),
        ),
        in_specs=[hbm] * 4 + [vmem] * 10,
        out_specs=[vmem] * 4,
        scratch_shapes=[
            pltpu.VMEM((seqs, seg, width), bf16),
            pltpu.VMEM((2 * seqs, EDGE, width), bf16),
            pltpu.VMEM((width, lanes), bf16),
            pltpu.VMEM((width, value_width), bf16),
            pltpu.VMEM((depth, out_width), bf16),
            pltpu.VMEM((width, 2 * heads), bf16),
            pltpu.VMEM((seg, seg), bf16),
            pltpu.VMEM((seg + 16, lanes), f32),
            pltpu.VMEM((seg, value_width), bf16),
            pltpu.VMEM((2 * heads, seg), f32),
            pltpu.VMEM((seqs, sp_count, cols, lanes), bf16),
            pltpu.VMEM((seqs, sp_count, cols, lanes), bf16),
            pltpu.VMEM((seqs, NOTE_ROWS, lanes), f32),
            pltpu.VMEM((seqs, sp_count, NOTE_ROWS, lanes), f32),
            pltpu.VMEM((2, seqs, lanes), f32),
            pltpu.VMEM((2, seqs, lanes), f32),
            pltpu.VMEM((total, seqs, features), f32),
            pltpu.VMEM((total, seqs, features), f32),
            pltpu.SemaphoreType.DMA((seqs,)),
            pltpu.SemaphoreType.DMA((2 * seqs,)),
            pltpu.SemaphoreType.DMA((3,)),
            pltpu.SemaphoreType.DMA((seqs, sp_count)),
            pltpu.SemaphoreType.DMA((seqs, sp_count)),
            pltpu.SemaphoreType.DMA((seqs, sp_count)),
            pltpu.SemaphoreType.DMA((seqs, sp_count)),
            pltpu.SemaphoreType.DMA((2,)),
            pltpu.SemaphoreType.DMA((2,)),
            pltpu.SemaphoreType.DMA((total,)),
            pltpu.SemaphoreType.DMA((total,)),
        ],
        compiler_params=pltpu.CompilerParams(
            collective_id=0, has_side_effects=True, vmem_limit_bytes=60 * 2**20
        ),
    )(
        prompt,
        key_weight,
        value_weight,
        out_weight.reshape(depth, out_width),
        input_gate_weight.T,
        forget_gate_weight.T,
        forget_bias.reshape(1, heads),
        key_taps,
        extra_decay.transpose(0, 2, 1),
        new_query,
        new_key,
        new_value,
        new_input_gate,
        new_forget_gate,
    )
    return (memory.transpose(0, 1, 3, 2).astype(bf16), normer.astype(bf16), peak, read)


def solution(mesh):
    placed = (
        P(None, "sp", None),
        P(None, "tp"),
        P(None, "tp"),
        P(None, "tp"),
        P(None, "tp"),
        P("tp"),
        P(None, "tp"),
        P(None, "sp", "tp"),
        P(None, "tp", None),
        P(None, "tp", None),
        P(None, "tp", "sp"),
        P(None, "tp"),
        P(None, "tp"),
        P("tp", "sp", None),
    )
    return jax.shard_map(
        body,
        mesh=mesh,
        in_specs=placed,
        out_specs=(
            P(None, "tp", None, "sp"),
            P(None, "tp", "sp"),
            P(None, "tp"),
            P(None, ("sp", "tp")),
        ),
        check_vma=False,
    )
```

```python
import functools

import jax
import jax.numpy as jnp
from jax import lax
from jax.experimental import pallas as pl
from jax.experimental.pallas import tpu as pltpu
from jax.sharding import PartitionSpec as P

EDGE = 16
NOTE_ROWS = 4
SMALL = 10


def log_sigmoid(x):
    return jnp.minimum(x, 0.0) - jnp.log1p(jnp.exp(-jnp.abs(x)))


def three_parts(x):
    high = x.astype(jnp.bfloat16).astype(jnp.float32)
    rest = x - high
    middle = rest.astype(jnp.bfloat16).astype(jnp.float32)
    return jnp.concatenate([high, middle, rest - middle], axis=0).astype(jnp.bfloat16)


def kernel(
    sp_count,
    tp_count,
    prompt,
    key_weight,
    value_weight,
    out_weight,
    *rest,
):
    operands, rest = rest[:SMALL], rest[SMALL:]
    outs, rest = rest[:4], rest[4:]
    held, rest = rest[:SMALL], rest[SMALL:]
    work(sp_count, tp_count, prompt, key_weight, value_weight, out_weight, operands, *held, *outs, *rest)


def work(
    sp_count,
    tp_count,
    prompt,
    key_weight,
    value_weight,
    out_weight,
    operands,
    input_weight,
    forget_weight,
    bias,
    taps,
    extra,
    new_query,
    new_key,
    new_value,
    new_input,
    new_forget,
    memory_out,
    norm_out,
    peak_out,
    read_out,
    rows,
    edges,
    wk,
    wv,
    wo,
    wg,
    later,
    padded,
    values,
    gates,
    share,
    shares,
    note,
    notes,
    halo_out,
    halo_in,
    parts_out,
    parts_in,
    small_sem,
    row_sem,
    edge_sem,
    weight_sem,
    share_send,
    share_recv,
    note_send,
    note_recv,
    halo_send,
    halo_recv,
    part_send,
    part_recv,
):
    seqs, seg, width = rows.shape
    lanes = wk.shape[1]
    heads = bias.shape[1]
    key_size = lanes // heads
    value_size = wv.shape[1] // heads
    cols = value_size // sp_count
    total = sp_count * tp_count
    sp, tp = lax.axis_index("sp"), lax.axis_index("tp")
    me = sp * tp_count + tp
    f32, bf16 = jnp.float32, jnp.bfloat16

    def device(j):
        return {"sp": j // tp_count, "tp": lax.rem(j, tp_count)}

    barrier = pltpu.get_barrier_semaphore()

    def greet(o, carry):
        j = lax.rem(me + o, total)
        pl.semaphore_signal(
            barrier, inc=1, device_id=device(j), device_id_type=pl.DeviceIdType.MESH
        )
        return carry

    key_copy = pltpu.make_async_copy(key_weight, wk, weight_sem.at[0])
    value_copy = pltpu.make_async_copy(value_weight, wv, weight_sem.at[1])
    out_copy = pltpu.make_async_copy(out_weight, wo, weight_sem.at[2])
    edge_copies = [
        pltpu.make_async_copy(
            prompt.at[s, pl.ds(start, EDGE)], edges.at[2 * s + side], edge_sem.at[2 * s + side]
        )
        for s in range(seqs)
        for side, start in enumerate((0, seg - EDGE))
    ]
    smalls = (
        input_weight,
        forget_weight,
        bias,
        taps,
        extra,
        new_query,
        new_key,
        new_value,
        new_input,
        new_forget,
    )
    small_copies = [
        pltpu.make_async_copy(source, here, small_sem.at[i])
        for i, (source, here) in enumerate(zip(operands, smalls))
    ]
    for copy in small_copies:
        copy.start()
    for copy in edge_copies:
        copy.start()
    key_copy.start()
    pltpu.make_async_copy(prompt.at[0], rows.at[0], row_sem.at[0]).start()
    value_copy.start()
    lax.fori_loop(1, total, greet, 0)

    place = lax.broadcasted_iota(jnp.int32, (seg, seg), 0)
    other = lax.broadcasted_iota(jnp.int32, (seg, seg), 1)
    later[...] = jnp.where(place > other, 1.0, 0.0).astype(bf16)
    for copy in small_copies:
        copy.wait()
    gate_rows = jnp.concatenate(
        [forget_weight[...].astype(f32), input_weight[...].astype(f32)], axis=0
    )
    wg[...] = gate_rows.T.astype(bf16)

    def column(x):
        size = x.shape[1]
        down = lax.broadcasted_iota(jnp.int32, (size, size), 0)
        across = lax.broadcasted_iota(jnp.int32, (size, size), 1)
        return jnp.sum(jnp.where(down == across, x, 0.0), axis=1, keepdims=True)

    bias_column = column(bias[...])

    for copy in edge_copies:
        copy.wait()
    key_copy.wait()
    edge_keys = jnp.dot(
        edges[...].reshape(2 * seqs * EDGE, width), wk[...], preferred_element_type=f32
    )
    edge_keys = edge_keys.astype(bf16).astype(f32)
    for s in range(seqs):
        first = 2 * s * EDGE
        last = first + 2 * EDGE - 1
        halo_out[0, s : s + 1, :] = edge_keys[last : last + 1]
        halo_out[1, s : s + 1, :] = edge_keys[first : first + 1]
    pl.semaphore_wait(barrier, total - 1)
    after = lax.rem(sp + 1, sp_count)
    before = lax.rem(sp + sp_count - 1, sp_count)
    halo_copies = [
        pltpu.make_async_remote_copy(
            src_ref=halo_out.at[i],
            dst_ref=halo_in.at[i],
            send_sem=halo_send.at[i],
            recv_sem=halo_recv.at[i],
            device_id={"sp": to, "tp": tp},
            device_id_type=pl.DeviceIdType.MESH,
        )
        for i, to in enumerate((after, before))
    ]
    for copy in halo_copies:
        copy.start()
    value_copy.wait()

    lane_head = lax.broadcasted_iota(jnp.int32, (1, lanes), 1) // key_size
    tap = taps[...].astype(f32)

    def by_head(x):
        out = jnp.zeros((x.shape[0], lanes), f32)
        for h in range(heads):
            out = jnp.where(lane_head == h, x[:, h : h + 1], out)
        return out

    def columns_by_head(x):
        row = lax.broadcasted_iota(jnp.int32, (heads, lanes), 0)
        return jnp.sum(jnp.where(row == lane_head, x, 0.0), axis=0, keepdims=True)

    def share_copy(s, q, slot):
        return pltpu.make_async_remote_copy(
            src_ref=share.at[s, q],
            dst_ref=shares.at[s, slot],
            send_sem=share_send.at[s, q],
            recv_sem=share_recv.at[s, slot],
            device_id={"sp": q, "tp": tp},
            device_id_type=pl.DeviceIdType.MESH,
        )

    def note_copy(s, q, slot):
        return pltpu.make_async_remote_copy(
            src_ref=note.at[s],
            dst_ref=notes.at[s, slot],
            send_sem=note_send.at[s, q],
            recv_sem=note_recv.at[s, slot],
            device_id={"sp": q, "tp": tp},
            device_id_type=pl.DeviceIdType.MESH,
        )

    block = min(256, seg)

    def project(i, s):
        at = pl.ds(pl.multiple_of(i * block, block), block)
        x = rows[s, at, :]
        key_raw = jnp.dot(x, wk[...], preferred_element_type=f32)
        padded[pl.ds(pl.multiple_of(i * block + 8, 8), block), :] = key_raw.astype(bf16).astype(f32)
        values[at, :] = jnp.dot(x, wv[...], preferred_element_type=f32).astype(bf16)
        gate = jnp.dot(x, wg[...], preferred_element_type=f32)
        gates[:, at] = gate.T.astype(bf16).astype(f32)
        return s

    def sequence(s, carry):
        pltpu.make_async_copy(prompt.at[s], rows.at[s], row_sem.at[s]).wait()

        @pl.when(s + 1 < seqs)
        def _():
            pltpu.make_async_copy(prompt.at[s + 1], rows.at[s + 1], row_sem.at[s + 1]).start()

        @pl.when(s + 1 == seqs)
        def _():
            out_copy.start()

        lax.fori_loop(0, seg // block, project, s)

        @pl.when(s == 0)
        def _():
            for copy in halo_copies:
                copy.wait()

        zero = jnp.zeros((1, lanes), f32)
        padded[7:8, :] = jnp.where(sp == 0, zero, halo_in[0, pl.ds(s, 1), :])
        padded[seg + 8 : seg + 9, :] = jnp.where(
            sp == sp_count - 1, zero, halo_in[1, pl.ds(s, 1), :]
        )
        mixed = (
            tap[0:1] * padded[7 : seg + 7, :]
            + tap[1:2] * padded[8 : seg + 8, :]
            + tap[2:3] * padded[9 : seg + 9, :]
        )
        key_rows = (mixed * jax.nn.sigmoid(mixed) * key_size ** (-0.5)).astype(bf16)

        gate = gates[...]
        log_forget = log_sigmoid(gate[:heads] + bias_column) + extra[s]
        sums = jnp.dot(three_parts(log_forget), later[...], preferred_element_type=f32)
        suffix = sums[:heads] + sums[heads : 2 * heads] + sums[2 * heads :]
        gate_log = gate[heads:] + suffix
        seg_total = jnp.sum(log_forget, axis=1, keepdims=True)
        top = jnp.max(gate_log, axis=1, keepdims=True)
        scale = jnp.exp(gate_log - top)
        scale_columns = jnp.concatenate([scale, jnp.zeros((8 - heads, seg), f32)], axis=0).T

        over = (((0,), (0,)), ((), ()))
        memory = jnp.zeros((value_size, lanes), f32)
        for h in range(heads):
            value = values[:, h * value_size : (h + 1) * value_size].astype(f32)
            weighted = (value * scale_columns[:, h : h + 1]).astype(bf16)
            outer = lax.dot_general(weighted, key_rows, over, preferred_element_type=f32)
            memory = jnp.where(lane_head == h, outer, memory)
        normers = jnp.dot(three_parts(scale), key_rows, preferred_element_type=f32)
        row_head = lax.rem(lax.broadcasted_iota(jnp.int32, normers.shape, 0), heads)
        normer = jnp.sum(jnp.where(row_head == lane_head, normers, 0.0), axis=0, keepdims=True)
        note[s, 0:1, :] = normer
        note[s, 1:2, :] = columns_by_head(seg_total)
        note[s, 2:3, :] = columns_by_head(top)
        note[s, 3:4, :] = jnp.zeros((1, lanes), f32)
        for q in range(sp_count):
            share[s, q] = memory[q * cols : (q + 1) * cols].astype(bf16)
        shares[s, sp] = share[s, sp]
        notes[s, sp] = note[s]

        def send(o, c):
            q = lax.rem(sp + o, sp_count)
            note_copy(s, q, sp).start()
            share_copy(s, q, sp).start()
            return c

        return lax.fori_loop(1, sp_count, send, carry)

    lax.fori_loop(0, seqs, sequence, 0)

    queries, keys = (
        jnp.concatenate([ref[:, h, :].astype(f32) for h in range(heads)], axis=1)
        for ref in (new_query, new_key)
    )
    inputs = [by_head(new_input[s : s + 1, :]) for s in range(seqs)]
    forgets = [log_sigmoid(by_head(new_forget[s : s + 1, :])) for s in range(seqs)]
    fresh = []
    for s in range(seqs):
        out = jnp.zeros((cols, lanes), f32)
        for h in range(heads):
            out = jnp.where(lane_head == h, column(new_value[s, h : h + 1, :].astype(f32)), out)
        fresh.append(out)


    depth = heads * cols
    lane = lax.broadcasted_iota(jnp.int32, (depth, 128), 1)
    reads = jnp.zeros((depth, 128), f32)
    for s in range(seqs):
        for o in range(1, sp_count):
            q = lax.rem(sp + o, sp_count)
            note_copy(s, q, q).wait_recv()
            share_copy(s, q, q).wait_recv()
        tail = jnp.zeros((1, lanes), f32)
        tops = [None] * sp_count
        for d in reversed(range(sp_count)):
            tops[d] = notes[s, d, 2:3, :] + tail
            tail = tail + notes[s, d, 1:2, :]
        peak = functools.reduce(jnp.maximum, tops)
        memory = jnp.zeros((cols, lanes), f32)
        normer = jnp.zeros((1, lanes), f32)
        for d in range(sp_count):
            factor = jnp.exp(tops[d] - peak)
            memory = memory + factor * shares[s, d].astype(f32)
            normer = normer + factor * notes[s, d, 0:1, :]
        key_cols = norm_out.shape[2]
        turned = pltpu.roll(
            jnp.broadcast_to(normer, (8, lanes)), lax.rem(lanes - sp * key_cols, lanes), 1
        )
        for h in range(heads):
            start = h * key_size
            memory_out[s, h] = memory[:, start : start + key_size]
            norm_out[s, h : h + 1, :] = turned[0:1, start : start + key_cols]
            peak_out[s : s + 1, h : h + 1] = peak[:, start : start + 1]
        query, key = queries[s : s + 1], keys[s : s + 1]
        input_new, forget_new = inputs[s], forgets[s]
        new_peak = jnp.maximum(forget_new + peak, input_new)
        old_scale = jnp.exp(forget_new + peak - new_peak)
        new_scale = jnp.exp(input_new - new_peak)
        numer = query * (old_scale * memory + new_scale * key * fresh[s])
        denom = query * (old_scale * normer + new_scale * key)
        found = []
        for h in range(heads):
            top = jnp.sum(jnp.where(lane_head == h, numer, 0.0), axis=1, keepdims=True)
            under = jnp.sum(jnp.where(lane_head == h, denom, 0.0), axis=1, keepdims=True)
            found.append(top / jnp.maximum(jnp.abs(under), 1.0))
        reads = jnp.where(lane == s, jnp.concatenate(found, axis=0), reads)
    if depth < 128:
        reads = jnp.concatenate([reads, jnp.zeros((128 - depth, 128), f32)], axis=0)
    out_copy.wait()
    left = reads.T[:8, :depth].astype(bf16)
    partial = jnp.dot(left, wo[...], preferred_element_type=f32)
    features = read_out.shape[1]
    for j in range(total):
        parts_out[j] = partial[:seqs, j * features : (j + 1) * features]
    parts_in[me] = parts_out[me]

    def part_copy(j, slot):
        return pltpu.make_async_remote_copy(
            src_ref=parts_out.at[j],
            dst_ref=parts_in.at[slot],
            send_sem=part_send.at[j],
            recv_sem=part_recv.at[slot],
            device_id=device(j),
            device_id_type=pl.DeviceIdType.MESH,
        )

    others = [lax.rem(me + o, total) for o in range(1, total)]
    for j in others:
        part_copy(j, me).start()
    for s in range(seqs):
        for o in range(1, sp_count):
            q = lax.rem(sp + o, sp_count)
            note_copy(s, q, q).wait_send()
            share_copy(s, q, q).wait_send()
    for j in others:
        part_copy(j, j).wait_send()
    for j in others:
        part_copy(j, j).wait_recv()
    read_out[...] = jnp.sum(parts_in[...], axis=0).astype(bf16)


def finish(*refs):
    for source, out in zip(refs[:4], refs[4:]):
        out[...] = source[...].astype(out.dtype)


def body(
    prompt,
    key_weight,
    value_weight,
    input_gate_weight,
    forget_gate_weight,
    forget_bias,
    key_taps,
    extra_decay,
    new_query,
    new_key,
    new_value,
    new_input_gate,
    new_forget_gate,
    out_weight,
):
    f32, bf16 = jnp.float32, jnp.bfloat16
    sp_count, tp_count = lax.axis_size("sp"), lax.axis_size("tp")
    total = sp_count * tp_count
    seqs, seg, width = prompt.shape
    heads, key_size = new_key.shape[1:]
    lanes = heads * key_size
    cols = new_value.shape[2]
    value_width = value_weight.shape[1]
    depth = heads * cols
    out_width = out_weight.shape[2]
    features = out_width // total

    smalls = (
        input_gate_weight.T,
        forget_gate_weight.T,
        forget_bias.reshape(1, heads),
        key_taps,
        extra_decay.transpose(0, 2, 1),
        new_query,
        new_key,
        new_value,
        new_input_gate,
        new_forget_gate,
    )
    vmem = pl.BlockSpec(memory_space=pltpu.VMEM)
    hbm = pl.BlockSpec(memory_space=pl.ANY)
    memory, normer, peak, read = pl.pallas_call(
        functools.partial(kernel, sp_count, tp_count),
        out_shape=(
            jax.ShapeDtypeStruct((seqs, heads, cols, key_size), f32),
            jax.ShapeDtypeStruct((seqs, heads, key_size // sp_count), f32),
            jax.ShapeDtypeStruct((seqs, heads), f32),
            jax.ShapeDtypeStruct((seqs, features), bf16),
        ),
        in_specs=[hbm] * (4 + SMALL),
        out_specs=[vmem] * 4,
        scratch_shapes=[pltpu.VMEM(x.shape, x.dtype) for x in smalls]
        + [
            pltpu.VMEM((seqs, seg, width), bf16),
            pltpu.VMEM((2 * seqs, EDGE, width), bf16),
            pltpu.VMEM((width, lanes), bf16),
            pltpu.VMEM((width, value_width), bf16),
            pltpu.VMEM((depth, out_width), bf16),
            pltpu.VMEM((width, 2 * heads), bf16),
            pltpu.VMEM((seg, seg), bf16),
            pltpu.VMEM((seg + 16, lanes), f32),
            pltpu.VMEM((seg, value_width), bf16),
            pltpu.VMEM((2 * heads, seg), f32),
            pltpu.VMEM((seqs, sp_count, cols, lanes), bf16),
            pltpu.VMEM((seqs, sp_count, cols, lanes), bf16),
            pltpu.VMEM((seqs, NOTE_ROWS, lanes), f32),
            pltpu.VMEM((seqs, sp_count, NOTE_ROWS, lanes), f32),
            pltpu.VMEM((2, seqs, lanes), f32),
            pltpu.VMEM((2, seqs, lanes), f32),
            pltpu.VMEM((total, seqs, features), f32),
            pltpu.VMEM((total, seqs, features), f32),
            pltpu.SemaphoreType.DMA((SMALL,)),
            pltpu.SemaphoreType.DMA((seqs,)),
            pltpu.SemaphoreType.DMA((2 * seqs,)),
            pltpu.SemaphoreType.DMA((3,)),
            pltpu.SemaphoreType.DMA((seqs, sp_count)),
            pltpu.SemaphoreType.DMA((seqs, sp_count)),
            pltpu.SemaphoreType.DMA((seqs, sp_count)),
            pltpu.SemaphoreType.DMA((seqs, sp_count)),
            pltpu.SemaphoreType.DMA((2,)),
            pltpu.SemaphoreType.DMA((2,)),
            pltpu.SemaphoreType.DMA((total,)),
            pltpu.SemaphoreType.DMA((total,)),
        ],
        compiler_params=pltpu.CompilerParams(
            collective_id=0, has_side_effects=True, vmem_limit_bytes=60 * 2**20
        ),
    )(
        prompt,
        key_weight,
        value_weight,
        out_weight.reshape(depth, out_width),
        *smalls,
    )
    memory, normer, peak, read = pl.pallas_call(
        finish,
        out_shape=(
            jax.ShapeDtypeStruct(memory.shape, bf16),
            jax.ShapeDtypeStruct(normer.shape, bf16),
            jax.ShapeDtypeStruct(peak.shape, f32),
            jax.ShapeDtypeStruct(read.shape, bf16),
        ),
        in_specs=[vmem] * 4,
        out_specs=[vmem] * 4,
    )(memory, normer, peak, read)
    return memory.transpose(0, 1, 3, 2), normer, peak, read


def solution(mesh):
    placed = (
        P(None, "sp", None),
        P(None, "tp"),
        P(None, "tp"),
        P(None, "tp"),
        P(None, "tp"),
        P("tp"),
        P(None, "tp"),
        P(None, "sp", "tp"),
        P(None, "tp", None),
        P(None, "tp", None),
        P(None, "tp", "sp"),
        P(None, "tp"),
        P(None, "tp"),
        P("tp", "sp", None),
    )
    return jax.shard_map(
        body,
        mesh=mesh,
        in_specs=placed,
        out_specs=(
            P(None, "tp", None, "sp"),
            P(None, "tp", "sp"),
            P(None, "tp"),
            P(None, ("sp", "tp")),
        ),
        check_vma=False,
    )
```
